32 devices in a mesh: sp: 16 (over z, y, x), tp: 2 (over core).
Axes of the slice: x: 2, y: 2, z: 4, core: 2. Of those that a mesh axis runs over, the one named last changes fastest.
Arguments:
- residual: bfloat16 [3072, 2048], P(('sp', 'tp')), may hold values from -6 to 6
- queries: bfloat16 [3072, 1024], P('sp', 'tp'), may hold values from -6 to 6
- key_pairs: bfloat16 [3072, 1024], P('sp', 'tp'), may hold values from -6 to 6
- values: bfloat16 [3072, 1024], P('sp', 'tp'), may hold values from -6 to 6
- second_weight: float32 [8], P('tp'), may hold values from 0.3 to 0.8
- head_gain: float32 [1024], P('tp'), may hold values from 0.1 to 1.9
- out_weight: bfloat16 [1024, 2048], P('tp'), may hold values from -0.1875 to 0.1875
- norm_gain: float32 [2048], replicated, may hold values from 0.1 to 1.9
- up_weight: bfloat16 [2048, 5632], P('sp', 'tp'), may hold values from -0.125 to 0.125
- gate_weight: bfloat16 [2048, 5632], P('sp', 'tp'), may hold values from -0.125 to 0.125
- conv_weight: float32 [3, 5632], P(None, 'tp'), may hold values from -3.5 to 3.5
- conv_bias: float32 [5632], P('tp'), may hold values from -3 to 3
- down_weight: bfloat16 [5632, 2048], P('tp', 'sp'), may hold values from -0.078125 to 0.078125
Outputs:
- layer_out: bfloat16 [3072, 2048], P(('sp', 'tp'))
The draws below stay inside these ranges and needn't reach their ends.
All inputs are finite; a program needn't handle non-finite values.
Results may differ from the reference program's by a relative error of at most 0.017.
Values may be sent and summed in bfloat16 or wider, within the bound.
A program may use at most 128 MiB of HBM per device.

```python
import math
import jax
import jax.numpy as jnp
from jax import lax

D = 2048
HEADS = 8
HD = 64
VD = 128
FF = 5632
KW = 3
TOKENS = 3072
N_TP = 2


def plant_pairs(key):
    base_key = jax.random.fold_in(key, 101)
    key_q, key_k = jax.random.split(base_key, 2)
    width_all = HEADS * 2 * HD
    query_draw = jax.random.normal(key_q, (TOKENS, width_all), jnp.float32) * 1.3
    key_draw = jax.random.normal(key_k, (TOKENS, width_all), jnp.float32) * 1.3
    return (jnp.clip(query_draw, -6.0, 6.0), jnp.clip(key_draw, -6.0, 6.0))


def draw_queries(key, part):
    return plant_pairs(key)[0].astype(jnp.bfloat16)


def draw_key_pairs(key, part):
    return plant_pairs(key)[1].astype(jnp.bfloat16)


def steps_of(stream_key, extent, cuts, least, high):
    loudness = 1.0
    for position, blocks in cuts:
        draws = jax.random.uniform(jax.random.fold_in(jax.random.fold_in(stream_key, 6), position), (blocks,), jnp.float32, least / len(cuts), high / len(cuts))
        loudness = loudness * jnp.repeat(jnp.exp(draws), extent[position] // blocks).reshape((-1,) + (1,) * (len(extent) - 1 - position))
    return loudness


def normal_values(key, extent, spread, bound, cuts=(), held_as=jnp.bfloat16):
    entries = jax.random.normal(key, extent, jnp.float32) * spread
    if len(cuts) > 0:
        entries = steps_of(key, extent, cuts, -0.22, 0.18) * entries
    return jnp.clip(entries, min=-bound, max=bound).astype(held_as)


def setup_inputs(seed: int = 0) -> dict:
    key_list = jax.random.split(jax.random.key(seed), 14)
    return {
        "residual": normal_values(key_list[0], (TOKENS, D), 1.0, 6.0, ((0, 32),)),
        "queries": draw_queries(jax.random.fold_in(key_list[13], 71), 0),
        "key_pairs": draw_key_pairs(jax.random.fold_in(key_list[13], 71), 0),
        "values": normal_values(key_list[3], (TOKENS, HEADS * VD), 1.0, 6.0, ((0, 16), (1, 2))),
        "second_weight": jnp.clip(0.3 + 0.5 * jax.random.uniform(key_list[4], (HEADS,), jnp.float32) ** steps_of(key_list[4], (HEADS,), ((0, 2),), -0.2, 0.2), 0.3, 0.8),
        "head_gain": jnp.clip(1.0 + 0.18 * jax.random.normal(key_list[5], (HEADS * VD,), jnp.float32), 0.1, 1.9),
        "out_weight": normal_values(key_list[6], (HEADS * VD, D), (HEADS * VD) ** -0.5, 0.1875, ((0, 2),)),
        "norm_gain": jnp.clip(1.0 + 0.18 * jax.random.normal(key_list[7], (D,), jnp.float32), 0.1, 1.9),
        "up_weight": normal_values(key_list[8], (D, FF), D ** -0.5, 0.125, ((0, 16), (1, 2))),
        "gate_weight": normal_values(key_list[9], (D, FF), D ** -0.5, 0.125, ((0, 16), (1, 2))),
        "conv_weight": normal_values(key_list[10], (KW, FF), KW ** -0.5, 3.5, ((1, 2),), jnp.float32),
        "conv_bias": normal_values(key_list[11], (FF,), 0.5, 3.0, ((0, 2),), jnp.float32),
        "down_weight": normal_values(key_list[12], (FF, D), FF ** -0.5, 0.078125, ((0, 2), (1, 16))),
    }


eps = 1e-05
neg_fill = -1e+30

def normalize(rows_in, gain):
    values_f = rows_in.astype(jnp.float32)
    scale_inv = lax.rsqrt(lax.optimization_barrier(jnp.mean(values_f * values_f, axis=-1, keepdims=True)) + eps)
    return (values_f * scale_inv * gain).astype(jnp.bfloat16)

def reference(residual, queries, key_pairs, values, second_weight, head_gain, out_weight, norm_gain, up_weight, gate_weight, conv_weight, conv_bias, down_weight):
    block_size = math.gcd(TOKENS, 512)
    block_count = TOKENS // block_size
    query_all = queries.astype(jnp.float32).reshape(TOKENS, HEADS, 2, HD)
    key_all = key_pairs.astype(jnp.float32).reshape(TOKENS, HEADS, 2, HD)
    value_all = values.astype(jnp.float32).reshape(TOKENS, HEADS, VD)
    key_pos = jnp.arange(TOKENS).astype(jnp.int32)
    gain_heads = head_gain.reshape(HEADS, VD)

    def attend_block(index_block):
        first = (index_block * block_size).astype(jnp.int32)
        query_block = lax.dynamic_slice_in_dim(query_all, first, block_size, 0)
        positions = first + jnp.arange(block_size).astype(jnp.int32)
        scores = jnp.einsum('qhmd,khmd->hmqk', query_block, key_all) * HD ** (-0.5)
        visible = key_pos[None, :] <= positions[:, None]
        scores = jnp.where(visible, scores, neg_fill)
        maxima = lax.optimization_barrier(jnp.max(scores, axis=-1, keepdims=True))
        exp_scores = jnp.where(visible, jnp.exp(scores - maxima), jnp.float32(0.0))
        totals = lax.optimization_barrier(jnp.sum(exp_scores, axis=-1))
        rounded = exp_scores.astype(jnp.bfloat16).astype(jnp.float32)
        weighted = jnp.einsum('hmqk,khe->hmqe', rounded, value_all)
        diff = weighted[:, 0] / totals[:, 0, :, None] - second_weight[:, None, None] * weighted[:, 1] / totals[:, 1, :, None]
        diff = jnp.transpose(diff, (1, 0, 2))
        scale_inv = lax.rsqrt(lax.optimization_barrier(jnp.mean(diff * diff, axis=-1, keepdims=True)) + eps)
        normed_heads = diff * scale_inv * gain_heads * 0.8
        return normed_heads.reshape(block_size, HEADS * VD).astype(jnp.bfloat16)
    attended = lax.map(attend_block, jnp.arange(block_count).astype(jnp.int32)).reshape(TOKENS, HEADS * VD)
    group_rows = HEADS * VD // N_TP
    proj_sum = jnp.zeros((TOKENS, D), jnp.float32)
    for group in range(N_TP):
        part_prod = jnp.dot(attended[:, group * group_rows:(group + 1) * group_rows], out_weight[group * group_rows:(group + 1) * group_rows], preferred_element_type=jnp.float32)
        proj_sum = proj_sum + part_prod.astype(jnp.bfloat16).astype(jnp.float32)
    proj = proj_sum.astype(jnp.bfloat16)
    mid = (residual.astype(jnp.float32) + proj.astype(jnp.float32)).astype(jnp.bfloat16)
    normed = normalize(mid, norm_gain)
    up_proj = jnp.dot(normed, up_weight, preferred_element_type=jnp.float32).astype(jnp.bfloat16)
    gate_proj = jnp.dot(normed, gate_weight, preferred_element_type=jnp.float32).astype(jnp.bfloat16)
    padded = jnp.pad(up_proj.astype(jnp.float32), ((KW - 1, 0), (0, 0)))
    conv_out = jnp.zeros((TOKENS, FF), jnp.float32) + conv_bias
    for tap in range(KW):
        conv_out = conv_out + conv_weight[tap] * padded[tap:tap + TOKENS]
    hidden = (jax.nn.silu(conv_out) * gate_proj.astype(jnp.float32)).astype(jnp.bfloat16)
    group_units = FF // N_TP
    ffn_sum = jnp.zeros((TOKENS, D), jnp.float32)
    for group in range(N_TP):
        part_prod = jnp.dot(hidden[:, group * group_units:(group + 1) * group_units], down_weight[group * group_units:(group + 1) * group_units], preferred_element_type=jnp.float32)
        ffn_sum = ffn_sum + part_prod.astype(jnp.bfloat16).astype(jnp.float32)
    ffn_out = ffn_sum.astype(jnp.bfloat16)
    return (mid.astype(jnp.float32) + ffn_out.astype(jnp.float32)).astype(jnp.bfloat16)
```

```python
import functools

import jax
import jax.numpy as jnp
from jax import lax
from jax.experimental import pallas as pl
from jax.experimental.pallas import tpu as pltpu
from jax.sharding import PartitionSpec as P

MESH = pl.DeviceIdType.MESH
VMEM_LIMIT = 60 * 1024 * 1024

HD = 64
VD = 128


eps = 1e-05
neg_fill = -1e30


def from_behind(value, axis, steps):
    count = lax.axis_size(axis)
    leading, last = (max(0, -steps), min(count, count - steps))
    return lax.ppermute(value, axis, [(source, source + steps) for source in range(leading, last)])


def normalize(rows_in, gain):
    values_f = rows_in.astype(jnp.float32)
    scale_inv = lax.rsqrt(jnp.mean(values_f * values_f, axis=-1, keepdims=True) + eps)
    return (values_f * scale_inv * gain).astype(jnp.bfloat16)


def attend(queries, key_pairs, values, second_weight, head_gain):
    tok_rows = queries.shape[0]
    head_count = second_weight.shape[0]
    sp_index = lax.axis_index("sp")
    query = queries.reshape(tok_rows, head_count, 2, HD)
    query_pos = sp_index * tok_rows + jnp.arange(tok_rows)
    last_query = (sp_index + 1) * tok_rows
    initial = (
        jnp.full((head_count, 2, tok_rows), neg_fill, jnp.float32),
        jnp.zeros((head_count, 2, tok_rows), jnp.float32),
        jnp.zeros((head_count, 2, tok_rows, VD), jnp.float32),
    )
    key_piece = lax.all_gather(key_pairs, "sp", axis=0, tiled=True)
    value_piece = lax.all_gather(values, "sp", axis=0, tiled=True)
    piece_len = key_piece.shape[0]

    def compute(state_in):
        maxima, totals, weighted = state_in
        key_rows = key_piece.reshape(piece_len, head_count, 2, HD)
        value_rows = value_piece.reshape(piece_len, head_count, VD)
        scores = jnp.einsum(
            "qhmd,khmd->hmqk", query, key_rows, preferred_element_type=jnp.float32
        ) * HD ** (-0.5)
        visible = jnp.arange(piece_len)[None, :] <= query_pos[:, None]
        scores = jnp.where(visible, scores, neg_fill)
        new_max = jnp.maximum(maxima, jnp.max(scores, axis=-1))
        exp_scores = jnp.where(visible, jnp.exp(scores - new_max[..., None]), jnp.float32(0.0))
        totals = jnp.sum(exp_scores, axis=-1)
        weighted = jnp.einsum(
            "hmqk,khe->hmqe",
            exp_scores.astype(jnp.bfloat16),
            value_rows,
            preferred_element_type=jnp.float32,
        )
        return (new_max, totals, weighted)

    def keep_state(state_in):
        return state_in

    maxima, totals, weighted = lax.cond(jnp.int32(0) < last_query, compute, keep_state, initial)
    diff = (
        weighted[:, 0] / totals[:, 0, :, None]
        - second_weight[:, None, None] * weighted[:, 1] / totals[:, 1, :, None]
    )
    diff = jnp.transpose(diff, (1, 0, 2))
    scale_inv = lax.rsqrt(jnp.mean(diff * diff, axis=-1, keepdims=True) + eps)
    attended = (
        (diff * scale_inv * head_gain.reshape(head_count, VD) * 0.8)
        .reshape(tok_rows, head_count * VD)
        .astype(jnp.bfloat16)
    )
    return attended


def local(
    residual,
    queries,
    key_pairs,
    values,
    second_weight,
    head_gain,
    out_weight,
    norm_gain,
    up_weight,
    gate_weight,
    conv_weight,
    conv_bias,
    down_weight,
):
    tok_rows = queries.shape[0]
    ff_local = up_weight.shape[1]
    attended = attend(queries, key_pairs, values, second_weight, head_gain)
    proj = lax.psum_scatter(
        jnp.dot(attended, out_weight, preferred_element_type=jnp.float32).astype(jnp.bfloat16),
        "tp",
        scatter_dimension=0,
        tiled=True,
    )
    mid = (residual.astype(jnp.float32) + proj.astype(jnp.float32)).astype(jnp.bfloat16)
    normed_all = lax.all_gather(normalize(mid, norm_gain), "tp", axis=0, tiled=True)
    up_sum = jnp.dot(
        normed_all,
        lax.all_gather(up_weight, "sp", axis=0, tiled=True),
        preferred_element_type=jnp.float32,
    )
    gate_sum = jnp.dot(
        normed_all,
        lax.all_gather(gate_weight, "sp", axis=0, tiled=True),
        preferred_element_type=jnp.float32,
    )
    up_proj = up_sum.astype(jnp.bfloat16)
    gate_proj = gate_sum.astype(jnp.bfloat16)
    taps = conv_weight.shape[0]
    rim_rows = from_behind(up_proj[tok_rows - (taps - 1) :], "sp", 1)
    extended = jnp.concatenate((rim_rows, up_proj), axis=0)
    conv_out = jnp.zeros((tok_rows, ff_local), jnp.float32) + conv_bias[None, :]
    for tap in range(taps):
        conv_out = conv_out + conv_weight[tap][None, :] * extended[tap : tap + tok_rows].astype(
            jnp.float32
        )
    hidden = (jax.nn.silu(conv_out) * gate_proj.astype(jnp.float32)).astype(jnp.bfloat16)
    down_all = lax.all_gather(down_weight, "sp", axis=1, tiled=True)
    ffn_out = lax.psum_scatter(
        jnp.dot(hidden, down_all, preferred_element_type=jnp.float32).astype(jnp.bfloat16),
        "tp",
        scatter_dimension=0,
        tiled=True,
    )
    return (mid.astype(jnp.float32) + ffn_out.astype(jnp.float32)).astype(jnp.bfloat16)


def greet(n, me, t):
    barrier = pltpu.get_barrier_semaphore()

    def signal(k, carry):
        pl.semaphore_signal(
            barrier, inc=1, device_id={"sp": lax.rem(me + k, n)}, device_id_type=MESH
        )
        return carry

    lax.fori_loop(1, n, signal, 0)
    pl.semaphore_signal(barrier, inc=1, device_id={"tp": 1 - t}, device_id_type=MESH)
    pl.semaphore_wait(barrier, n)


def to_sp(src, dst, send, recv, dest):
    return pltpu.make_async_remote_copy(
        src_ref=src, dst_ref=dst, send_sem=send, recv_sem=recv,
        device_id={"sp": dest}, device_id_type=MESH,
    )


def to_tp(src, dst, send, recv, dest):
    return pltpu.make_async_remote_copy(
        src_ref=src, dst_ref=dst, send_sem=send, recv_sem=recv,
        device_id={"tp": dest}, device_id_type=MESH,
    )


def gather_kernel(
    n, att, ow, res, gain, wu, wg, up, gate, mid,
    buf, pbuf, prbuf, psem, send, recv, fsend, frecv,
):
    me = lax.axis_index("sp")
    t = lax.axis_index("tp")
    half = res.shape[0]
    rows = 2 * half
    mine = pl.ds(pl.multiple_of(t * half, half), half)
    theirs = pl.ds(pl.multiple_of((1 - t) * half, half), half)
    greet(n, me, t)
    pbuf[...] = jnp.dot(att[theirs, :], ow[...], preferred_element_type=jnp.float32).astype(
        jnp.bfloat16
    )
    swap = to_tp(pbuf, prbuf, psem.at[0], psem.at[1], 1 - t)
    swap.start()
    own = jnp.dot(att[mine, :], ow[...], preferred_element_type=jnp.float32).astype(jnp.bfloat16)
    swap.wait()
    proj = (own.astype(jnp.float32) + prbuf[...].astype(jnp.float32)).astype(jnp.bfloat16)
    mid_v = (res[...].astype(jnp.float32) + proj.astype(jnp.float32)).astype(jnp.bfloat16)
    mid[...] = mid_v
    mid_f = mid_v.astype(jnp.float32)
    inv = lax.rsqrt(jnp.mean(mid_f * mid_f, axis=-1, keepdims=True) + eps)
    buf[0, mine, :] = (mid_f * inv * gain[...]).astype(jnp.bfloat16)

    def spread(k):
        return to_sp(
            buf.at[0, mine], buf.at[k, mine], send.at[k], recv.at[k], lax.rem(me + k, n)
        )

    def forward(k):
        return to_tp(buf.at[k, mine], buf.at[k, mine], fsend.at[k], frecv.at[k], 1 - t)

    def arrived(k):
        return to_tp(buf.at[k, theirs], buf.at[k, theirs], fsend.at[k], frecv.at[k], 1 - t)

    forward(0).start()

    def start(k, carry):
        spread(k).start()
        return carry

    lax.fori_loop(1, n, start, 0)

    def compute(k):
        arrived(k).wait_recv()
        first = pl.multiple_of(lax.rem(me - k + n, n) * rows, rows)
        block = buf[k]
        up[pl.ds(first, rows), :] = jnp.dot(
            block, wu[...], preferred_element_type=jnp.float32
        ).astype(jnp.bfloat16)
        gate[pl.ds(first, rows), :] = jnp.dot(
            block, wg[...], preferred_element_type=jnp.float32
        ).astype(jnp.bfloat16)

    def step(k, carry):
        spread(k).wait_recv()
        forward(k).start()
        compute(k - 1)
        return carry

    lax.fori_loop(1, n, step, 0)
    compute(n - 1)

    def drain(k, carry):
        spread(k).wait_send()
        forward(k).wait_send()
        return carry

    forward(0).wait_send()
    lax.fori_loop(1, n, drain, 0)


def scatter_kernel(
    n, hid, down, mid, out, pb, pr, sb, rb, psend, precv, send, recv,
):
    me = lax.axis_index("sp")
    t = lax.axis_index("tp")
    half = mid.shape[0]
    rows = 2 * half
    greet(n, me, t)

    def swap(k):
        return to_tp(pb.at[k], pr.at[k], psend.at[k], precv.at[k], 1 - t)

    def away(k):
        return to_sp(sb.at[k], rb.at[k], send.at[k], recv.at[k], lax.rem(me + k, n))

    def product(k):
        first = lax.rem(me + k, n) * rows
        theirs = pl.ds(pl.multiple_of(first + (1 - t) * half, half), half)
        mine = pl.ds(pl.multiple_of(first + t * half, half), half)
        pb[k] = jnp.dot(hid[theirs, :], down[...], preferred_element_type=jnp.float32).astype(
            jnp.bfloat16
        )
        swap(k).start()
        sb[k] = jnp.dot(hid[mine, :], down[...], preferred_element_type=jnp.float32).astype(
            jnp.bfloat16
        )

    def combine(k):
        swap(k).wait_recv()
        sb[k] = (sb[k].astype(jnp.float32) + pr[k].astype(jnp.float32)).astype(jnp.bfloat16)

    product(1)

    def step(k, carry):
        product(k)
        combine(k - 1)
        away(k - 1).start()
        return carry

    lax.fori_loop(2, n, step, 0)
    product(0)
    combine(n - 1)
    away(n - 1).start()
    combine(0)

    total = sb[0].astype(jnp.float32)

    def add(k, total):
        away(k).wait_recv()
        return total + rb[k].astype(jnp.float32)

    acc = lax.fori_loop(1, n, add, total)
    ffn = acc.astype(jnp.bfloat16).astype(jnp.float32)
    out[...] = (mid[...].astype(jnp.float32) + ffn).astype(jnp.bfloat16)

    def drain(k, carry):
        away(k).wait_send()
        swap(k).wait_send()
        return carry

    swap(0).wait_send()
    lax.fori_loop(1, n, drain, 0)


def vm(count):
    return [pl.BlockSpec(memory_space=pltpu.VMEM)] * count


def params(cid):
    return pltpu.CompilerParams(
        collective_id=cid, has_side_effects=True, vmem_limit_bytes=VMEM_LIMIT
    )


def gather_rows(n, att, ow, res, gain, wu, wg):
    half, width = res.shape
    units = wu.shape[1]
    rows = 2 * half
    bf = jnp.bfloat16
    dma = pltpu.SemaphoreType.DMA
    return pl.pallas_call(
        functools.partial(gather_kernel, n),
        out_shape=(
            jax.ShapeDtypeStruct((n * rows, units), bf),
            jax.ShapeDtypeStruct((n * rows, units), bf),
            jax.ShapeDtypeStruct((half, width), bf),
        ),
        in_specs=vm(6),
        out_specs=tuple(vm(3)),
        scratch_shapes=[
            pltpu.VMEM((n, rows, width), bf),
            pltpu.VMEM((half, width), bf),
            pltpu.VMEM((half, width), bf),
            dma((2,)), dma((n,)), dma((n,)), dma((n,)), dma((n,)),
        ],
        compiler_params=params(1),
        name="gather_rows",
    )(att, ow, res, gain[None, :], wu, wg)


def scatter_rows(n, hid, down, mid):
    half, width = mid.shape
    bf = jnp.bfloat16
    dma = pltpu.SemaphoreType.DMA
    block = pltpu.VMEM((n, half, width), bf)
    return pl.pallas_call(
        functools.partial(scatter_kernel, n),
        out_shape=jax.ShapeDtypeStruct((half, width), bf),
        in_specs=vm(3),
        out_specs=vm(1)[0],
        scratch_shapes=[block, block, block, block, dma((n,)), dma((n,)), dma((n,)), dma((n,))],
        compiler_params=params(2),
        name="scatter_rows",
    )(hid, down, mid)


def moving_rows(
    n,
    residual,
    queries,
    key_pairs,
    values,
    second_weight,
    head_gain,
    out_weight,
    norm_gain,
    up_weight,
    gate_weight,
    conv_weight,
    conv_bias,
    down_weight,
):
    sp_index = lax.axis_index("sp")
    units = up_weight.shape[1] // n
    taps = conv_weight.shape[0]
    wu = lax.all_to_all(up_weight, "sp", split_axis=1, concat_axis=0, tiled=True)
    wg = lax.all_to_all(gate_weight, "sp", split_axis=1, concat_axis=0, tiled=True)
    wd = lax.all_to_all(down_weight, "sp", split_axis=0, concat_axis=1, tiled=True)
    cw = lax.dynamic_slice_in_dim(conv_weight, sp_index * units, units, 1)
    cb = lax.dynamic_slice_in_dim(conv_bias, sp_index * units, units, 0)
    attended = attend(queries, key_pairs, values, second_weight, head_gain)
    up, gate, mid = gather_rows(n, attended, out_weight, residual, norm_gain, wu, wg)
    count = up.shape[0]
    extended = jnp.pad(up, ((taps - 1, 0), (0, 0)))
    conv_out = jnp.zeros((count, units), jnp.float32) + cb[None, :]
    for tap in range(taps):
        conv_out = conv_out + cw[tap][None, :] * extended[tap : tap + count].astype(jnp.float32)
    hidden = (jax.nn.silu(conv_out) * gate.astype(jnp.float32)).astype(jnp.bfloat16)
    return scatter_rows(n, hidden, wd, mid)


def choose(n_sp, n_tp):
    def body(residual, queries, *rest):
        up_weight = rest[6]
        token_count = queries.shape[0] * n_sp
        width = residual.shape[1]
        moves_rows = (
            n_tp == 2
            and 2 * token_count < 3 * n_tp * up_weight.shape[1]
            and up_weight.shape[1] % n_sp == 0
            and n_sp % rest[2].shape[0] == 0
        )
        if moves_rows:
            return moving_rows(n_sp, residual, queries, *rest)
        return local(residual, queries, *rest)

    return body


def solution(mesh):
    return jax.shard_map(
        choose(mesh.shape["sp"], mesh.shape["tp"]),
        mesh=mesh,
        in_specs=(
            P(("sp", "tp"), None),
            P("sp", "tp"),
            P("sp", "tp"),
            P("sp", "tp"),
            P("tp"),
            P("tp"),
            P("tp", None),
            P(),
            P("sp", "tp"),
            P("sp", "tp"),
            P(None, "tp"),
            P("tp"),
            P("tp", "sp"),
        ),
        out_specs=P(("sp", "tp"), None),
        check_vma=False,
    )
```

```python
import functools
import math

import jax
import jax.numpy as jnp
from jax import lax
from jax.experimental import pallas as pl
from jax.experimental.pallas import tpu as pltpu
from jax.sharding import PartitionSpec as P

MESH = pl.DeviceIdType.MESH
VMEM_LIMIT = 60 * 1024 * 1024

HD = 64
VD = 128


eps = 1e-05
neg_fill = -1e30


def from_behind(value, axis, steps):
    count = lax.axis_size(axis)
    leading, last = (max(0, -steps), min(count, count - steps))
    return lax.ppermute(value, axis, [(source, source + steps) for source in range(leading, last)])


def normalize(rows_in, gain):
    values_f = rows_in.astype(jnp.float32)
    scale_inv = lax.rsqrt(jnp.mean(values_f * values_f, axis=-1, keepdims=True) + eps)
    return (values_f * scale_inv * gain).astype(jnp.bfloat16)


def attend(queries, key_pairs, values, second_weight, head_gain):
    tok_rows = queries.shape[0]
    head_count = second_weight.shape[0]
    sp_index = lax.axis_index("sp")
    query = queries.reshape(tok_rows, head_count, 2, HD)
    query_pos = sp_index * tok_rows + jnp.arange(tok_rows)
    last_query = (sp_index + 1) * tok_rows
    initial = (
        jnp.full((head_count, 2, tok_rows), neg_fill, jnp.float32),
        jnp.zeros((head_count, 2, tok_rows), jnp.float32),
        jnp.zeros((head_count, 2, tok_rows, VD), jnp.float32),
    )
    key_piece = lax.all_gather(key_pairs, "sp", axis=0, tiled=True)
    value_piece = lax.all_gather(values, "sp", axis=0, tiled=True)
    piece_len = key_piece.shape[0]

    def compute(state_in):
        maxima, totals, weighted = state_in
        key_rows = key_piece.reshape(piece_len, head_count, 2, HD)
        value_rows = value_piece.reshape(piece_len, head_count, VD)
        scores = jnp.einsum(
            "qhmd,khmd->hmqk", query, key_rows, preferred_element_type=jnp.float32
        ) * HD ** (-0.5)
        visible = jnp.arange(piece_len)[None, :] <= query_pos[:, None]
        scores = jnp.where(visible, scores, neg_fill)
        new_max = jnp.maximum(maxima, jnp.max(scores, axis=-1))
        exp_scores = jnp.where(visible, jnp.exp(scores - new_max[..., None]), jnp.float32(0.0))
        totals = jnp.sum(exp_scores, axis=-1)
        weighted = jnp.einsum(
            "hmqk,khe->hmqe",
            exp_scores.astype(jnp.bfloat16),
            value_rows,
            preferred_element_type=jnp.float32,
        )
        return (new_max, totals, weighted)

    def keep_state(state_in):
        return state_in

    maxima, totals, weighted = lax.cond(jnp.int32(0) < last_query, compute, keep_state, initial)
    diff = (
        weighted[:, 0] / totals[:, 0, :, None]
        - second_weight[:, None, None] * weighted[:, 1] / totals[:, 1, :, None]
    )
    diff = jnp.transpose(diff, (1, 0, 2))
    scale_inv = lax.rsqrt(jnp.mean(diff * diff, axis=-1, keepdims=True) + eps)
    attended = (
        (diff * scale_inv * head_gain.reshape(head_count, VD) * 0.8)
        .reshape(tok_rows, head_count * VD)
        .astype(jnp.bfloat16)
    )
    return attended


def local(
    residual,
    queries,
    key_pairs,
    values,
    second_weight,
    head_gain,
    out_weight,
    norm_gain,
    up_weight,
    gate_weight,
    conv_weight,
    conv_bias,
    down_weight,
):
    tok_rows = queries.shape[0]
    ff_local = up_weight.shape[1]
    attended = attend(queries, key_pairs, values, second_weight, head_gain)
    proj = lax.psum_scatter(
        jnp.dot(attended, out_weight, preferred_element_type=jnp.float32).astype(jnp.bfloat16),
        "tp",
        scatter_dimension=0,
        tiled=True,
    )
    mid = (residual.astype(jnp.float32) + proj.astype(jnp.float32)).astype(jnp.bfloat16)
    normed_all = lax.all_gather(normalize(mid, norm_gain), "tp", axis=0, tiled=True)
    up_sum = jnp.dot(
        normed_all,
        lax.all_gather(up_weight, "sp", axis=0, tiled=True),
        preferred_element_type=jnp.float32,
    )
    gate_sum = jnp.dot(
        normed_all,
        lax.all_gather(gate_weight, "sp", axis=0, tiled=True),
        preferred_element_type=jnp.float32,
    )
    up_proj = up_sum.astype(jnp.bfloat16)
    gate_proj = gate_sum.astype(jnp.bfloat16)
    taps = conv_weight.shape[0]
    rim_rows = from_behind(up_proj[tok_rows - (taps - 1) :], "sp", 1)
    extended = jnp.concatenate((rim_rows, up_proj), axis=0)
    conv_out = jnp.zeros((tok_rows, ff_local), jnp.float32) + conv_bias[None, :]
    for tap in range(taps):
        conv_out = conv_out + conv_weight[tap][None, :] * extended[tap : tap + tok_rows].astype(
            jnp.float32
        )
    hidden = (jax.nn.silu(conv_out) * gate_proj.astype(jnp.float32)).astype(jnp.bfloat16)
    down_all = lax.all_gather(down_weight, "sp", axis=1, tiled=True)
    ffn_out = lax.psum_scatter(
        jnp.dot(hidden, down_all, preferred_element_type=jnp.float32).astype(jnp.bfloat16),
        "tp",
        scatter_dimension=0,
        tiled=True,
    )
    return (mid.astype(jnp.float32) + ffn_out.astype(jnp.float32)).astype(jnp.bfloat16)


def greet(n, me, t):
    barrier = pltpu.get_barrier_semaphore()

    def signal(k, carry):
        pl.semaphore_signal(
            barrier, inc=1, device_id={"sp": lax.rem(me + k, n)}, device_id_type=MESH
        )
        return carry

    lax.fori_loop(1, n, signal, 0)
    pl.semaphore_signal(barrier, inc=1, device_id={"tp": 1 - t}, device_id_type=MESH)
    pl.semaphore_wait(barrier, n)


def to_sp(src, dst, send, recv, dest):
    return pltpu.make_async_remote_copy(
        src_ref=src, dst_ref=dst, send_sem=send, recv_sem=recv,
        device_id={"sp": dest}, device_id_type=MESH,
    )


def to_tp(src, dst, send, recv, dest):
    return pltpu.make_async_remote_copy(
        src_ref=src, dst_ref=dst, send_sem=send, recv_sem=recv,
        device_id={"tp": dest}, device_id_type=MESH,
    )


def gather_kernel(
    n, att, ow, res, gain, wu, wg, up, gate, mid,
    buf, pbuf, prbuf, psem, send, recv, fsend, frecv,
):
    me = lax.axis_index("sp")
    t = lax.axis_index("tp")
    half = res.shape[0]
    rows = 2 * half
    mine = pl.ds(pl.multiple_of(t * half, half), half)
    theirs = pl.ds(pl.multiple_of((1 - t) * half, half), half)
    greet(n, me, t)
    pbuf[...] = jnp.dot(att[theirs, :], ow[...], preferred_element_type=jnp.float32).astype(
        jnp.bfloat16
    )
    swap = to_tp(pbuf, prbuf, psem.at[0], psem.at[1], 1 - t)
    swap.start()
    own = jnp.dot(att[mine, :], ow[...], preferred_element_type=jnp.float32).astype(jnp.bfloat16)
    swap.wait()
    proj = (own.astype(jnp.float32) + prbuf[...].astype(jnp.float32)).astype(jnp.bfloat16)
    mid_v = (res[...].astype(jnp.float32) + proj.astype(jnp.float32)).astype(jnp.bfloat16)
    mid[...] = mid_v
    mid_f = mid_v.astype(jnp.float32)
    inv = lax.rsqrt(jnp.mean(mid_f * mid_f, axis=-1, keepdims=True) + eps)
    buf[0, mine, :] = (mid_f * inv * gain[...]).astype(jnp.bfloat16)

    p = plane_of(n)
    layers = n // p
    z, w = me // p, lax.rem(me, p)

    def column(a):
        dest = lax.rem(z + a, layers) * p + w
        return to_sp(buf.at[0, mine], buf.at[a * p, mine], send.at[a * p], recv.at[a * p], dest)

    def spread(a, b):
        slot = a * p + b
        dest = z * p + lax.rem(w + b, p)
        return to_sp(
            buf.at[a * p, mine], buf.at[slot, mine], send.at[slot], recv.at[slot], dest
        )

    def forward(k):
        return to_tp(buf.at[k, mine], buf.at[k, mine], fsend.at[k], frecv.at[k], 1 - t)

    def arrived(k):
        return to_tp(buf.at[k, theirs], buf.at[k, theirs], fsend.at[k], frecv.at[k], 1 - t)

    def relay(a):
        for b in range(1, p):
            spread(a, b).start()
        forward(a * p).start()

    def compute(a, b):
        arrived(a * p + b).wait_recv()
        source = lax.rem(z - a + layers, layers) * p + lax.rem(w - b + p, p)
        first = pl.multiple_of(source * rows, rows)
        block = buf[a * p + b]
        up[pl.ds(first, rows), :] = jnp.dot(
            block, wu[...], preferred_element_type=jnp.float32
        ).astype(jnp.bfloat16)
        gate[pl.ds(first, rows), :] = jnp.dot(
            block, wg[...], preferred_element_type=jnp.float32
        ).astype(jnp.bfloat16)

    for a in range(1, layers):
        column(a).start()
    relay(0)

    def stage(a, carry):
        @pl.when(a + 1 < layers)
        def _():
            column(a + 1).wait_recv()
            relay(a + 1)

        def step(b, carry):
            spread(a, b).wait_recv()
            forward(a * p + b).start()
            compute(a, b - 1)
            return carry

        lax.fori_loop(1, p, step, 0)
        compute(a, p - 1)
        return carry

    lax.fori_loop(0, layers, stage, 0)

    def drain(a, carry):
        for b in range(1, p):
            spread(a, b).wait_send()
            forward(a * p + b).wait_send()
        forward(a * p).wait_send()
        return carry

    lax.fori_loop(0, layers, drain, 0)
    for a in range(1, layers):
        column(a).wait_send()


def scatter_kernel(
    n, hid, down, mid, out, pb, pr, sb, rb, zb, cb, psend, precv, send, recv, zsend, zrecv,
):
    me = lax.axis_index("sp")
    t = lax.axis_index("tp")
    half = mid.shape[0]
    rows = 2 * half
    p = plane_of(n)
    layers = n // p
    z, w = me // p, lax.rem(me, p)
    greet(n, me, t)

    def place(i):
        return lax.rem(i // p + 1, layers), lax.rem(lax.rem(i, p) + 1, p)

    def swap(i):
        a, b = place(i)
        slot = a * p + b
        return to_tp(pb.at[slot], pr.at[slot], psend.at[slot], precv.at[slot], 1 - t)

    def across(a, b):
        slot = a * p + b
        dest = z * p + lax.rem(w + b, p)
        return to_sp(sb.at[slot], rb.at[slot], send.at[slot], recv.at[slot], dest)

    def column(a):
        dest = lax.rem(z + a, layers) * p + w
        return to_sp(zb.at[a], cb.at[a], zsend.at[a], zrecv.at[a], dest)

    def product(i):
        a, b = place(i)
        slot = a * p + b
        first = (lax.rem(z + a, layers) * p + lax.rem(w + b, p)) * rows
        theirs = pl.ds(pl.multiple_of(first + (1 - t) * half, half), half)
        mine = pl.ds(pl.multiple_of(first + t * half, half), half)
        pb[slot] = jnp.dot(hid[theirs, :], down[...], preferred_element_type=jnp.float32).astype(
            jnp.bfloat16
        )
        swap(i).start()
        sb[slot] = jnp.dot(hid[mine, :], down[...], preferred_element_type=jnp.float32).astype(
            jnp.bfloat16
        )

    def combine(i):
        a, b = place(i)
        slot = a * p + b
        swap(i).wait_recv()
        sb[slot] = (sb[slot].astype(jnp.float32) + pr[slot].astype(jnp.float32)).astype(
            jnp.bfloat16
        )

        @pl.when(b != 0)
        def _():
            across(a, b).start()

    def plane_sum(a):
        acc = sb[a * p].astype(jnp.float32)
        for b in range(1, p):
            across(a, b).wait_recv()
            acc = acc + rb[a * p + b].astype(jnp.float32)
        return acc

    product(0)

    def step(i, carry):
        product(i)
        combine(i - 1)

        @pl.when(jnp.logical_and(lax.rem(i, p) == p - 1, i >= p))
        def _():
            a = i // p
            zb[a] = plane_sum(a).astype(jnp.bfloat16)
            column(a).start()

        return carry

    lax.fori_loop(1, n, step, 0)
    combine(n - 1)
    acc = plane_sum(0)
    for a in range(1, layers):
        column(a).wait_recv()
        acc = acc + cb[a].astype(jnp.float32)
    ffn = acc.astype(jnp.bfloat16).astype(jnp.float32)
    out[...] = (mid[...].astype(jnp.float32) + ffn).astype(jnp.bfloat16)

    def drain(a, carry):
        for b in range(1, p):
            across(a, b).wait_send()
        for b in range(p):
            swap(a * p + b).wait_send()
        return carry

    lax.fori_loop(0, layers, drain, 0)
    for a in range(1, layers):
        column(a).wait_send()


def plane_of(n):
    return math.gcd(n, 4)


def vm(count):
    return [pl.BlockSpec(memory_space=pltpu.VMEM)] * count


def params(cid):
    return pltpu.CompilerParams(
        collective_id=cid, has_side_effects=True, vmem_limit_bytes=VMEM_LIMIT
    )


def gather_rows(n, att, ow, res, gain, wu, wg):
    half, width = res.shape
    units = wu.shape[1]
    rows = 2 * half
    bf = jnp.bfloat16
    dma = pltpu.SemaphoreType.DMA
    return pl.pallas_call(
        functools.partial(gather_kernel, n),
        out_shape=(
            jax.ShapeDtypeStruct((n * rows, units), bf),
            jax.ShapeDtypeStruct((n * rows, units), bf),
            jax.ShapeDtypeStruct((half, width), bf),
        ),
        in_specs=vm(6),
        out_specs=tuple(vm(3)),
        scratch_shapes=[
            pltpu.VMEM((n, rows, width), bf),
            pltpu.VMEM((half, width), bf),
            pltpu.VMEM((half, width), bf),
            dma((2,)), dma((n,)), dma((n,)), dma((n,)), dma((n,)),
        ],
        compiler_params=params(1),
        name="gather_rows",
    )(att, ow, res, gain[None, :], wu, wg)


def scatter_rows(n, hid, down, mid):
    half, width = mid.shape
    bf = jnp.bfloat16
    dma = pltpu.SemaphoreType.DMA
    layers = n // plane_of(n)
    block = pltpu.VMEM((n, half, width), bf)
    few = pltpu.VMEM((layers, half, width), bf)
    return pl.pallas_call(
        functools.partial(scatter_kernel, n),
        out_shape=jax.ShapeDtypeStruct((half, width), bf),
        in_specs=vm(3),
        out_specs=vm(1)[0],
        scratch_shapes=[block, block, block, block, few, few]
        + [dma((n,)), dma((n,)), dma((n,)), dma((n,)), dma((layers,)), dma((layers,))],
        compiler_params=params(2),
        name="scatter_rows",
    )(hid, down, mid)


def attention_kernel(
    n, heads, q, k, v, sw, gain, ub, gb, db, att, wu, wg, wd,
    qb, kb, vb, ob, qsend, qrecv, ksend, krecv, vsend, vrecv, osend, orecv,
    usend, urecv, gsend, grecv, dsend, drecv,
):
    me = lax.axis_index("sp")
    t = lax.axis_index("tp")
    rows = q.shape[0]
    depth = db.shape[2]
    groups = n // heads
    chunk = 2 * rows

    def cols(h):
        return pl.ds(pl.multiple_of(h * VD, VD), VD)

    def at(s):
        return pl.ds(pl.multiple_of(s * rows, rows), rows)

    def group_of(s):
        i, r = s // groups, lax.rem(s, groups)
        return jnp.where(lax.rem(i, 2) == 0, r, groups - 1 - r)

    head = lax.rem(me, heads)
    group = me // heads
    my_group = group_of(me)
    my_slot = me // groups
    greet(n, me, t)

    def query_copy(h):
        return to_sp(
            q.at[:, cols(h)], qb.at[my_slot], qsend.at[h], qrecv.at[my_slot], my_group * heads + h
        )

    def block_of(i):
        return i * groups + (group if i % 2 == 0 else groups - 1 - group)

    def query_wait(i):
        to_sp(qb.at[i], qb.at[i], qsend.at[0], qrecv.at[i], me).wait_recv()

    for h in range(heads):
        other = my_group * heads + h != me

        @pl.when(other)
        def _():
            query_copy(h).start()

        @pl.when(jnp.logical_not(other))
        def _():
            qb[my_slot] = q[:, cols(h)]

    def pair(d):
        dest = lax.rem(me + d, n)
        h = lax.rem(dest, heads)
        return (
            to_sp(k.at[:, cols(h)], kb.at[at(me)], ksend.at[d], krecv.at[d], dest),
            to_sp(v.at[:, cols(h)], vb.at[at(me)], vsend.at[d], vrecv.at[d], dest),
        )

    def weights(d):
        dest = lax.rem(me + d, n)
        wide = pl.ds(pl.multiple_of(me * depth, depth), depth)
        return (
            to_sp(ub.at[dest], wu.at[me], usend.at[d], urecv.at[d], dest),
            to_sp(gb.at[dest], wg.at[me], gsend.at[d], grecv.at[d], dest),
            to_sp(db.at[dest], wd.at[:, wide], dsend.at[d], drecv.at[d], dest),
        )

    def begin(make):
        def start(d, carry):
            for copy in make(d):
                copy.start()
            return carry

        lax.fori_loop(1, n, start, 0)

    def finish(make, sent):
        def wait(d, carry):
            for copy in make(d):
                if sent:
                    copy.wait_send()
                else:
                    copy.wait_recv()
            return carry

        lax.fori_loop(1, n, wait, 0)

    begin(pair)
    begin(weights)
    kb[at(me), :] = k[:, cols(head)]
    vb[at(me), :] = v[:, cols(head)]
    wu[me] = ub[me]
    wg[me] = gb[me]
    wd[:, pl.ds(pl.multiple_of(me * depth, depth), depth)] = db[me]
    for i in range(heads):

        @pl.when(block_of(i) != me)
        def _():
            query_wait(i)

    finish(pair, False)
    weight = sw[head]
    gain_row = gain[pl.ds(head, 1), :]
    lane = lax.broadcasted_iota(jnp.int32, (rows, VD), 1)

    def answer(i):
        return to_sp(
            ob.at[i], att.at[:, cols(head)], osend.at[i], orecv.at[head], block_of(i)
        )

    for i in range(heads):
        block = block_of(i)
        query = (qb[i].astype(jnp.float32) * HD ** (-0.5)).astype(jnp.bfloat16)
        zero = jnp.zeros_like(query)
        both = jnp.concatenate(
            (jnp.where(lane < HD, query, zero), jnp.where(lane < HD, zero, query)), axis=0
        )
        last = block // 2

        def visit(c, state, masked):
            top, total, acc = state
            span = pl.ds(pl.multiple_of(c * chunk, chunk), chunk)
            scores = lax.dot_general(
                both, kb[span, :], (((1,), (1,)), ((), ())), preferred_element_type=jnp.float32
            )
            if masked:
                row = lax.broadcasted_iota(jnp.int32, scores.shape, 0)
                row = jnp.where(row < rows, row, row - rows)
                col = lax.broadcasted_iota(jnp.int32, scores.shape, 1)
                visible = c * chunk + col <= block * rows + row
                scores = jnp.where(visible, scores, neg_fill)
            new_top = jnp.maximum(top, jnp.max(scores, axis=-1, keepdims=True))
            shrink = jnp.exp(top - new_top)
            exp_scores = jnp.exp(scores - new_top)
            total = total * shrink + jnp.sum(exp_scores, axis=-1, keepdims=True)
            acc = acc * shrink + jnp.dot(
                exp_scores.astype(jnp.bfloat16), vb[span, :], preferred_element_type=jnp.float32
            )
            return new_top, total, acc

        state = (
            jnp.full((2 * rows, 1), neg_fill, jnp.float32),
            jnp.zeros((2 * rows, 1), jnp.float32),
            jnp.zeros((2 * rows, VD), jnp.float32),
        )
        state = lax.fori_loop(0, last, lambda c, state: visit(c, state, False), state)
        top, total, acc = visit(last, state, True)
        mean_v = acc / total
        diff = mean_v[:rows] - weight * mean_v[rows:]
        inv = lax.rsqrt(jnp.mean(diff * diff, axis=-1, keepdims=True) + eps)
        result = (diff * inv * gain_row * 0.8).astype(jnp.bfloat16)

        @pl.when(block != me)
        def _():
            ob[i] = result
            answer(i).start()

        @pl.when(block == me)
        def _():
            att[:, cols(head)] = result

    for h in range(heads):
        other = my_group * heads + h != me

        @pl.when(other)
        def _():
            to_sp(ob.at[0], att.at[:, cols(h)], osend.at[0], orecv.at[h], me).wait_recv()
            query_copy(h).wait_send()

    for i in range(heads):

        @pl.when(block_of(i) != me)
        def _():
            answer(i).wait_send()

    finish(pair, True)
    finish(weights, False)
    finish(weights, True)


def attend_rows(n, q, k, v, second_weight, head_gain, up_weight, gate_weight, down_weight):
    rows, width = q.shape
    heads = second_weight.shape[0]
    depth, ff_local = up_weight.shape
    units = ff_local // n
    bf = jnp.bfloat16
    dma = pltpu.SemaphoreType.DMA
    ub = up_weight.reshape(depth, n, units).transpose(1, 0, 2)
    gb = gate_weight.reshape(depth, n, units).transpose(1, 0, 2)
    db = down_weight.reshape(n, units, depth)
    many = [dma((n,))]
    att, wu, wg, wd = pl.pallas_call(
        functools.partial(attention_kernel, n, heads),
        out_shape=(
            jax.ShapeDtypeStruct((rows, width), bf),
            jax.ShapeDtypeStruct((n, depth, units), bf),
            jax.ShapeDtypeStruct((n, depth, units), bf),
            jax.ShapeDtypeStruct((units, n * depth), bf),
        ),
        in_specs=vm(3) + [pl.BlockSpec(memory_space=pltpu.SMEM)] + vm(4),
        out_specs=tuple(vm(4)),
        scratch_shapes=[
            pltpu.VMEM((heads, rows, VD), bf),
            pltpu.VMEM((n * rows, VD), bf),
            pltpu.VMEM((n * rows, VD), bf),
            pltpu.VMEM((heads, rows, VD), bf),
            dma((heads,)), dma((heads,)),
        ]
        + many * 4
        + [dma((heads,)), dma((heads,))]
        + many * 6,
        compiler_params=params(0),
        name="attend_rows",
    )(q, k, v, second_weight, head_gain.reshape(heads, VD), ub, gb, db)
    return att, wu.reshape(n * depth, units), wg.reshape(n * depth, units), wd


def moving_rows(
    n,
    residual,
    queries,
    key_pairs,
    values,
    second_weight,
    head_gain,
    out_weight,
    norm_gain,
    up_weight,
    gate_weight,
    conv_weight,
    conv_bias,
    down_weight,
):
    sp_index = lax.axis_index("sp")
    units = up_weight.shape[1] // n
    taps = conv_weight.shape[0]
    cw = lax.dynamic_slice_in_dim(conv_weight, sp_index * units, units, 1)
    cb = lax.dynamic_slice_in_dim(conv_bias, sp_index * units, units, 0)
    attended, wu, wg, wd = attend_rows(
        n, queries, key_pairs, values, second_weight, head_gain, up_weight, gate_weight, down_weight
    )
    up, gate, mid = gather_rows(n, attended, out_weight, residual, norm_gain, wu, wg)
    count = up.shape[0]
    extended = jnp.pad(up, ((taps - 1, 0), (0, 0)))
    conv_out = jnp.zeros((count, units), jnp.float32) + cb[None, :]
    for tap in range(taps):
        conv_out = conv_out + cw[tap][None, :] * extended[tap : tap + count].astype(jnp.float32)
    hidden = (jax.nn.silu(conv_out) * gate.astype(jnp.float32)).astype(jnp.bfloat16)
    return scatter_rows(n, hidden, wd, mid)


def choose(n_sp, n_tp):
    def body(residual, queries, *rest):
        up_weight = rest[6]
        token_count = queries.shape[0] * n_sp
        width = residual.shape[1]
        moves_rows = (
            n_tp == 2
            and 2 * token_count < 3 * n_tp * up_weight.shape[1]
            and up_weight.shape[1] % n_sp == 0
            and n_sp % rest[2].shape[0] == 0
        )
        if moves_rows:
            return moving_rows(n_sp, residual, queries, *rest)
        return local(residual, queries, *rest)

    return body


def solution(mesh):
    return jax.shard_map(
        choose(mesh.shape["sp"], mesh.shape["tp"]),
        mesh=mesh,
        in_specs=(
            P(("sp", "tp"), None),
            P("sp", "tp"),
            P("sp", "tp"),
            P("sp", "tp"),
            P("tp"),
            P("tp"),
            P("tp", None),
            P(),
            P("sp", "tp"),
            P("sp", "tp"),
            P(None, "tp"),
            P("tp"),
            P("tp", "sp"),
        ),
        out_specs=P(("sp", "tp"), None),
        check_vma=False,
    )
```
